32 devices in a mesh: ep: 8 (over z, x), tp: 4 (over y, core).
Axes of the slice: x: 2, y: 2, z: 4, core: 2. Of those that a mesh axis runs over, the one named last changes fastest.
Arguments:
- tokens: bfloat16 [32, 2048], P('ep'), may hold values from -6 to 6
- norm_gain: bfloat16 [2048], replicated, may hold values from 0.099609375 to 1.8984375
- in_weight: bfloat16 [2048, 1024], P(None, 'tp'), may hold values from -0.125 to 0.125
- decay_rate: float32 [64, 64], P('tp'), may hold values from 0.05 to 1
- frequency: float32 [64, 64], P('tp'), may hold values from -3 to 3
- log_step: float32 [64], P('tp'), may hold values from -2.3 to 0.7
- input_real: float32 [64, 64, 16], P('tp'), may hold values from -1.75 to 1.75
- input_imag: float32 [64, 64, 16], P('tp'), may hold values from -1.75 to 1.75
- output_real: float32 [64, 16, 64], P('tp'), may hold values from -0.5 to 0.5
- output_imag: float32 [64, 16, 64], P('tp'), may hold values from -0.5 to 0.5
- skip_gain: float32 [1024], P('tp'), may hold values from -3 to 3
- state_real: float32 [32, 64, 64], P('ep', 'tp'), may hold values from -6 to 6
- state_imag: float32 [32, 64, 64], P('ep', 'tp'), may hold values from -6 to 6
- out_weight: bfloat16 [1024, 2048], P('tp'), may hold values from -0.1875 to 0.1875
- ffn_gain: bfloat16 [2048], replicated, may hold values from 0.099609375 to 1.8984375
- expert_ids: int32 [32, 2], replicated, may hold values from 0 to 7, all different within a row; in each aligned block of 4 rows (0 to 3, 4 to 7, ...) at most 2 rows name the same one
- route_weights: float32 [32, 2], P('ep'), may hold values from 0.2 to 1
- gate_weight: bfloat16 [2048, 65536], P(None, ('ep', 'tp')), may hold values from -0.125 to 0.125
- up_weight: bfloat16 [2048, 65536], P(None, ('ep', 'tp')), may hold values from -0.125 to 0.125
- down_weight: bfloat16 [65536, 2048], P('ep', 'tp'), may hold values from -0.0625 to 0.0625
Outputs:
- mixed: bfloat16 [32, 2048], P('ep', 'tp')
- new_real: float32 [32, 64, 64], P('ep', 'tp')
- new_imag: float32 [32, 64, 64], P('ep', 'tp')
The draws below stay inside these ranges and needn't reach their ends.
Inputs may be any that keep to these rules, and one draw needn't show every extreme that they name: `expert_ids`: the 2 experts of a row differ. In each aligned block of 4 rows (the rows of one index of ep) no expert is named by more than 2 rows, and in some blocks one expert is named by exactly 2 rows.
All inputs are finite; a program needn't handle non-finite values.
Results may differ from the reference program's by a relative error of at most 0.007.
Values may be sent and summed in bfloat16 or wider, within the bound.
A program may use at most 64 MiB of HBM per device.

```python
import math
import jax
import jax.numpy as jnp
import numpy as np
from jax import lax

D = 2048
S5W = 1024
GROUP = 16
STATE = 64
EXPERTS = 8
TOP = 2
FF = 8192
SEQ_DEV = 4
GROUPS = 64
CAP = 2
TOKENS = 32
SPAN = 1
N_EP = 8


def block_levels(stream_key, dims, cuts, low, largest):
    factor_of, own = 1.0, jax.random.fold_in(stream_key, 6)
    for position, shards_of in cuts:
        steps = jnp.exp(jax.random.uniform(jax.random.fold_in(own, position), (shards_of,), jnp.float32, low / len(cuts), largest / len(cuts)))
        factor_of = factor_of * jnp.repeat(steps, dims[position] // shards_of).reshape([-1 if axis == position else 1 for axis in range(len(dims))])
    return factor_of


def assign_block(key, own, number, rows, amount, top, most, slope):
    sequence = jax.random.permutation(key, amount)
    packed, ordinary = load_shares(amount, rows * top, most, slope, True), load_shares(amount, rows * top, most, slope, False)
    places = jnp.arange(amount)

    def named(sizes, turn):
        used = int((sizes > 0).sum())
        fixed = max(1, used // 4)
        moved = fixed + (places - fixed + turn * (used - fixed)) % max(1, amount - fixed)
        return jnp.zeros((amount,), jnp.int32).at[sequence[jnp.where(places < fixed, places, moved)]].set(jnp.asarray(sizes, jnp.int32))

    sizes = jnp.where(number % 4 == 0, named(packed, number // 4), named(ordinary, number - number // 4 - 1))
    mixed = jax.random.permutation(jax.random.fold_in(own, 3), amount)
    donor, taker = mixed[0:amount // 2 * 2:2], mixed[1:amount // 2 * 2:2]
    slack = jnp.minimum(sizes[donor] - 1, most - sizes[taker]) // 2
    slack = jnp.where((donor == sequence[0]) | (taker == sequence[0]) | (sizes[taker] == 0), 0, jnp.maximum(slack, 0))
    moved = jax.random.randint(jax.random.fold_in(own, 4), (amount // 2,), 0, 1 << 20) % (slack + 1)
    sizes = sizes.at[donor].add(-moved).at[taker].add(moved)
    members = jnp.searchsorted(jnp.cumsum(sizes), jnp.arange(rows * top), side="right").astype(jnp.int32)
    grid = members.reshape(top, rows).T
    grid = grid[jax.random.permutation(jax.random.fold_in(own, 1), rows)]
    turn = jax.random.randint(jax.random.fold_in(own, 2), (rows, 1), 0, top)
    return jnp.take_along_axis(grid, (jnp.arange(top)[None, :] + turn) % top, axis=1)


def load_shares(amount, total, bound, slope, full):
    loads = [(1 << 20) // math.isqrt(grade ** slope) + 1 for grade in range(1, amount + 1)]
    largest = bound if full else min(bound, max(-(-total // amount), total * loads[0] // sum(loads)))
    least = 1 if total - largest >= amount - 1 else 0
    counts, rest = [largest] + [least] * (amount - 1), total - largest - least * (amount - 1)
    while rest > 0:
        candidates = [i for i in range(1, amount) if counts[i] < largest] or [i for i in range(1, amount) if counts[i] < bound]
        pool, left = sum([loads[i] for i in candidates]), rest
        for i in candidates:
            more = min(bound - counts[i], max(1, left * loads[i] // pool), rest)
            counts[i] = counts[i] + more
            rest = rest - more
    return np.array(counts)


def bell_draw(stream_key, shape, spread, most, cuts=(), held_as=jnp.bfloat16):
    entries = jax.random.normal(stream_key, shape, jnp.float32) * spread
    if len(cuts) > 0:
        entries = block_levels(stream_key, shape, cuts, -0.22, 0.18) * entries
    return jnp.clip(entries, min=-most, max=most).astype(held_as)


def setup_inputs(seed: int = 0) -> dict:
    splits = jax.random.split(jax.random.key(seed), 21)
    tokens = bell_draw(splits[0], (TOKENS, D), 1.0, 6.0, ((0, 8),))
    norm_gain = jnp.clip(1.0 + 0.18 * jax.random.normal(splits[1], (D,), jnp.float32), 0.099609375, 1.8984375).astype(jnp.bfloat16)
    in_weight = bell_draw(splits[2], (D, S5W), D ** -0.5, 0.125, ((1, 4),))
    decay_rate = jnp.clip(jnp.exp(math.log(1.0) - 2.9957323 * jax.random.uniform(splits[3], (GROUPS, STATE), jnp.float32) ** block_levels(splits[3], (GROUPS, STATE), ((0, 4),), -0.2, 0.2)), 0.05, 1.0)
    frequency = jnp.clip(jax.random.uniform(splits[4], (GROUPS, STATE), jnp.float32, -3.0, 3.0) * block_levels(splits[4], (GROUPS, STATE), ((0, 4),), -0.4, 0.0), -3.0, 3.0)
    log_step = jnp.clip(-2.3 + 3 * jax.random.uniform(splits[5], (GROUPS,), jnp.float32) ** block_levels(splits[5], (GROUPS,), ((0, 4),), -0.2, 0.2), -2.3, 0.7)
    input_real = bell_draw(splits[6], (GROUPS, STATE, GROUP), 0.3, 1.75, ((0, 4),), jnp.float32)
    input_imag = bell_draw(splits[7], (GROUPS, STATE, GROUP), 0.3, 1.75, ((0, 4),), jnp.float32)
    output_real = bell_draw(splits[8], (GROUPS, GROUP, STATE), (2 * STATE) ** -0.5, 0.5, ((0, 4),), jnp.float32)
    output_imag = bell_draw(splits[9], (GROUPS, GROUP, STATE), (2 * STATE) ** -0.5, 0.5, ((0, 4),), jnp.float32)
    skip_gain = bell_draw(splits[10], (S5W,), 0.5, 3.0, ((0, 4),), jnp.float32)
    state_real = bell_draw(splits[11], (TOKENS, GROUPS, STATE), 1.0, 6.0, ((0, 8), (1, 4)), jnp.float32)
    state_imag = bell_draw(splits[12], (TOKENS, GROUPS, STATE), 1.0, 6.0, ((0, 8), (1, 4)), jnp.float32)
    out_weight = bell_draw(splits[13], (S5W, D), S5W ** -0.5, 0.1875, ((0, 4),))
    ffn_gain = jnp.clip(1.0 + 0.18 * jax.random.normal(splits[14], (D,), jnp.float32), 0.099609375, 1.8984375).astype(jnp.bfloat16)
    expert_ids_keys = jax.random.split(jax.random.fold_in(splits[15], 1), TOKENS // SEQ_DEV)
    expert_ids_turns = jax.random.permutation(jax.random.fold_in(splits[15], 3), TOKENS // SEQ_DEV)
    expert_ids = jax.vmap(lambda own, number: assign_block(jax.random.fold_in(splits[15], 2), own, number, SEQ_DEV, EXPERTS, TOP, CAP, 2))(expert_ids_keys, expert_ids_turns).reshape((TOKENS, TOP))
    route_weights = jnp.clip(0.2 + 0.8 * jax.random.uniform(splits[16], (TOKENS, TOP), jnp.float32) ** block_levels(splits[16], (TOKENS, TOP), ((0, 8),), -0.2, 0.2), 0.2, 1.0)
    gate_weight = bell_draw(splits[17], (D, EXPERTS * FF), D ** -0.5, 0.125, ((1, 32),))
    up_weight = bell_draw(splits[18], (D, EXPERTS * FF), D ** -0.5, 0.125, ((1, 32),))
    down_weight = bell_draw(splits[19], (EXPERTS * FF, D), FF ** -0.5, 0.0625, ((0, 8), (1, 4)))
    return {"tokens": tokens, "norm_gain": norm_gain, "in_weight": in_weight, "decay_rate": decay_rate, "frequency": frequency, "log_step": log_step, "input_real": input_real, "input_imag": input_imag, "output_real": output_real, "output_imag": output_imag, "skip_gain": skip_gain, "state_real": state_real, "state_imag": state_imag, "out_weight": out_weight, "ffn_gain": ffn_gain, "expert_ids": expert_ids, "route_weights": route_weights, "gate_weight": gate_weight, "up_weight": up_weight, "down_weight": down_weight}


EPSILON = 1e-06

def rms_scale(values, gain):
    floats = values.astype(jnp.float32)
    return floats * lax.rsqrt(lax.optimization_barrier(jnp.mean(floats * floats, axis=-1, keepdims=True)) + EPSILON) * gain.astype(jnp.float32)

def discretize(decay_rate, frequency, log_step, input_real, input_imag):
    step_size = jnp.exp(log_step)[:, None]
    lam_real = -decay_rate
    magnitude = jnp.exp(lam_real * step_size)
    turned = frequency * step_size
    bar_real = magnitude * jnp.cos(turned)
    bar_imag = magnitude * jnp.sin(turned)
    denom = lam_real * lam_real + frequency * frequency
    minus_one = bar_real - 1.0
    factor_real = (minus_one * lam_real + bar_imag * frequency) / denom
    factor_imag = (bar_imag * lam_real - minus_one * frequency) / denom
    b_real = factor_real[..., None] * input_real - factor_imag[..., None] * input_imag
    b_imag = factor_real[..., None] * input_imag + factor_imag[..., None] * input_real
    return (bar_real, bar_imag, b_real, b_imag)

def state_update(projected, state_real, state_imag, decay_rate, frequency, log_step, input_real, input_imag, output_real, output_imag, skip_gain):
    bar_real, bar_imag, b_real, b_imag = discretize(decay_rate, frequency, log_step, input_real, input_imag)
    count, groups, _ = state_real.shape
    high = lax.Precision.HIGHEST
    grouped = projected.astype(jnp.float32).reshape(count, groups, -1)
    drive_real = jnp.einsum('sgp,gnp->sgn', grouped, b_real, precision=high)
    drive_imag = jnp.einsum('sgp,gnp->sgn', grouped, b_imag, precision=high)
    new_real = bar_real * state_real - bar_imag * state_imag + drive_real
    new_imag = bar_real * state_imag + bar_imag * state_real + drive_imag
    readout = jnp.einsum('sgn,gpn->sgp', new_real, output_real, precision=high) - jnp.einsum('sgn,gpn->sgp', new_imag, output_imag, precision=high)
    readout = readout.reshape(count, -1) + skip_gain * grouped.reshape(count, -1)
    return (jax.nn.gelu(readout).astype(jnp.bfloat16), new_real, new_imag)

def reference(tokens, norm_gain, in_weight, decay_rate, frequency, log_step, input_real, input_imag, output_real, output_imag, skip_gain, state_real, state_imag, out_weight, ffn_gain, expert_ids, route_weights, gate_weight, up_weight, down_weight):
    normed_in = rms_scale(tokens, norm_gain).astype(jnp.bfloat16)
    projected = jnp.dot(normed_in, in_weight, preferred_element_type=jnp.float32).astype(jnp.bfloat16)
    activated, new_real, new_imag = state_update(projected, state_real, state_imag, decay_rate, frequency, log_step, input_real, input_imag, output_real, output_imag, skip_gain)
    delta = jnp.dot(activated, out_weight, preferred_element_type=jnp.float32)
    hidden_state = (tokens.astype(jnp.float32) + delta).astype(jnp.bfloat16)
    normed = rms_scale(hidden_state, ffn_gain).astype(jnp.bfloat16)
    limit = min(TOKENS, N_EP * CAP)
    piece = FF // SPAN

    def expert_block(carry, expert):
        hits = expert_ids == expert
        row_weight = lax.optimization_barrier(jnp.sum(jnp.where(hits, route_weights, 0.0), axis=1))
        used = jnp.any(hits, axis=1)
        indices = jnp.nonzero(used, size=limit, fill_value=0)[0].astype(jnp.int32)
        valid = jnp.arange(limit, dtype=jnp.int32) < jnp.sum(used.astype(jnp.int32))
        chosen = normed[indices]
        start = (expert * FF).astype(jnp.int32)
        gate_cols = lax.dynamic_slice_in_dim(gate_weight, start, FF, 1)
        up_cols = lax.dynamic_slice_in_dim(up_weight, start, FF, 1)
        down_rows = lax.dynamic_slice_in_dim(down_weight, start, FF, 0)
        gate_pre = jnp.dot(chosen, gate_cols, preferred_element_type=jnp.float32)
        up_pre = jnp.dot(chosen, up_cols, preferred_element_type=jnp.float32)
        expert_hidden = (jax.nn.silu(gate_pre) * up_pre).astype(jnp.bfloat16)

        def one_piece(index):
            first = (index * piece).astype(jnp.int32)
            units = lax.dynamic_slice_in_dim(expert_hidden, first, piece, 1)
            rows = lax.dynamic_slice_in_dim(down_rows, first, piece, 0)
            part = jnp.dot(units, rows, preferred_element_type=jnp.float32).astype(jnp.bfloat16)
            return lax.optimization_barrier(part).astype(jnp.float32)
        pieces = lax.map(one_piece, jnp.arange(SPAN, dtype=jnp.int32))
        expert_out = lax.optimization_barrier(jnp.sum(pieces, axis=0))
        scale = jnp.where(valid, row_weight[indices], 0.0)
        return (carry.at[indices].add(scale[:, None] * expert_out), None)
    routed, _ = lax.scan(expert_block, jnp.zeros(normed.shape, jnp.float32), jnp.arange(EXPERTS, dtype=jnp.int32))
    mixed = (hidden_state.astype(jnp.float32) + routed).astype(jnp.bfloat16)
    return (mixed, new_real, new_imag)
```

```python
import functools

import jax
import jax.numpy as jnp
from jax import lax
from jax.experimental import pallas as pl
from jax.experimental.pallas import tpu as pltpu
from jax.sharding import PartitionSpec as P

EXPERTS = 8
EPSILON = 1e-06
MESH = pl.DeviceIdType.MESH
F32, BF16 = jnp.float32, jnp.bfloat16
NT = (((1,), (1,)), ((), ()))


def rms_scale(floats, gain):
    return (
        floats
        * lax.rsqrt(jnp.mean(floats * floats, axis=-1, keepdims=True) + EPSILON)
        * gain.astype(F32)
    )


def mm(a, b):
    return jnp.dot(a, b, preferred_element_type=F32)


def iota(shape, axis):
    return lax.broadcasted_iota(jnp.int32, shape, axis)


def route_masks(ids, base, seqs, slots, owners, span, rows_first):
    shape = (owners * slots, 1) if rows_first else (1, owners * slots)
    place = iota(shape, 0 if rows_first else 1)
    expert, slot = place // (slots * span), place % slots
    count = jnp.zeros(shape, jnp.int32)
    masks = []
    for s in range(seqs):
        picks = []
        hit = jnp.zeros(shape, jnp.int32)
        for k in range(ids.shape[1]):
            same = jnp.where(expert == ids[base + s, k], 1, 0)
            picks.append(jnp.where(count == slot, same, 0))
            hit = hit + same
        masks.append(picks)
        count = count + hit
    return masks


def kernel(
    n_ep,
    n_tp,
    tokens_h,
    norm_gain_h,
    in_w_h,
    decay_h,
    freq_h,
    log_step_h,
    in_re_h,
    in_im_h,
    out_re_h,
    out_im_h,
    skip_h,
    st_re_h,
    st_im_h,
    out_w_h,
    ffn_gain_h,
    ids,
    weights,
    gate_h,
    up_h,
    down_h,
    mixed_o,
    new_re_o,
    new_im_o,
    tokens_v,
    norm_gain_v,
    in_w_v,
    decay_v,
    freq_v,
    log_step_v,
    in_re_v,
    in_im_v,
    out_re_v,
    out_im_v,
    skip_v,
    st_re_v,
    st_im_v,
    out_w_v,
    ffn_gain_v,
    gate_v,
    up_v,
    down_v,
    bt_v,
    part_v,
    hidden_v,
    xs_v,
    x_v,
    outg_v,
    recvd_v,
    hid_v,
    ys_v,
    retg_v,
    retd_v,
    load_sem,
    gate_sem,
    up_sem,
    down_sem,
    part_send,
    part_recv,
    disp_send,
    disp_recv,
    hid_send,
    hid_recv,
    ret_send,
    ret_recv,
):
    ep, tp = lax.axis_index("ep"), lax.axis_index("tp")
    chunks, _, cw = gate_v.shape
    seqs, width = tokens_v.shape
    groups, states = decay_v.shape
    chan = in_re_v.shape[2]
    slots = seqs // 2
    span = n_ep // EXPERTS
    rows = n_ep * slots
    quarter = down_v.shape[1]
    piece = chunks * cw

    def tp_peer(d):
        return (tp // 2 * 2 + d // 2 * 2) % n_tp + (tp % 2 + d % 2) % 2

    def ep_to(d):
        return (ep + d) % n_ep

    def ep_from(d):
        return (ep + n_ep - d) % n_ep

    pairs = [
        (tokens_h, tokens_v),
        (norm_gain_h, norm_gain_v),
        (in_w_h, in_w_v),
        (in_re_h, in_re_v),
        (in_im_h, in_im_v),
        (log_step_h, log_step_v),
        (decay_h, decay_v),
        (freq_h, freq_v),
        (st_re_h, st_re_v),
        (st_im_h, st_im_v),
        (out_re_h, out_re_v),
        (out_im_h, out_im_v),
        (skip_h, skip_v),
        (out_w_h, out_w_v),
        (ffn_gain_h, ffn_gain_v),
    ]
    loads = [pltpu.make_async_copy(a, b, load_sem.at[i]) for i, (a, b) in enumerate(pairs)]
    for load in loads:
        load.start()

    barrier = pltpu.get_barrier_semaphore()
    for d in range(1, n_tp):
        pl.semaphore_signal(barrier, inc=1, device_id={"tp": tp_peer(d)}, device_id_type=MESH)
    for d in range(1, n_ep):
        pl.semaphore_signal(barrier, inc=1, device_id={"ep": ep_to(d)}, device_id_type=MESH)

    def gate_copy(c):
        cols = pl.ds(pl.multiple_of(c * cw, cw), cw)
        return (
            pltpu.make_async_copy(gate_h.at[:, cols], gate_v.at[c], gate_sem.at[c]),
            pltpu.make_async_copy(up_h.at[:, cols], up_v.at[c], up_sem.at[c]),
        )

    def down_copy(p):
        part = pl.ds(pl.multiple_of(p * piece, piece), piece)
        return pltpu.make_async_copy(down_h.at[part], down_v.at[part], down_sem.at[p])

    for c in range(chunks):
        for copy in gate_copy(c):
            copy.start()
    for d in range(n_tp):
        down_copy(tp_peer(d)).start()

    for load in loads[3:8]:
        load.wait()
    ident = (iota((chan, chan), 0) == iota((chan, chan), 1)).astype(BF16)

    def turn(g, _):
        both = jnp.concatenate([in_re_v[g], in_im_v[g]], axis=0).astype(BF16)
        bt_v[g] = lax.dot_general(ident, both, NT, preferred_element_type=F32).astype(BF16)
        return 0

    lax.fori_loop(0, groups, turn, 0)
    eye = iota((groups, groups), 0) == iota((groups, groups), 1)
    step_size = jnp.sum(jnp.where(eye, jnp.exp(log_step_v[...]), 0.0), axis=1, keepdims=True)
    lam_real, frequency = -decay_v[...], freq_v[...]
    magnitude = jnp.exp(lam_real * step_size)
    turned = frequency * step_size
    bar_real = magnitude * jnp.cos(turned)
    bar_imag = magnitude * jnp.sin(turned)
    denom = lam_real * lam_real + frequency * frequency
    minus_one = bar_real - 1.0
    factor_real = (minus_one * lam_real + bar_imag * frequency) / denom
    factor_imag = (bar_imag * lam_real - minus_one * frequency) / denom

    def per_seq(values):
        return jnp.concatenate([values] * seqs, axis=0)

    for load in loads[0:3]:
        load.wait()
    floats = tokens_v[...].astype(F32)
    normed_in = rms_scale(floats, norm_gain_v[...]).astype(BF16)
    projected = mm(normed_in, in_w_v[...]).astype(BF16).astype(F32)
    channels = projected.shape[1]
    own = iota((groups, channels), 1) // chan == iota((groups, channels), 0)
    spread = jnp.concatenate(
        [
            jnp.where(own, jnp.broadcast_to(projected[s : s + 1], own.shape), 0.0)
            for s in range(seqs)
        ],
        axis=0,
    ).astype(BF16)
    drive = mm(spread, bt_v[...].reshape(channels, 2 * states))
    drive_real, drive_imag = drive[:, :states], drive[:, states:]
    for load in loads[8:13]:
        load.wait()
    sr = st_re_v[...].reshape(seqs * groups, states)
    si = st_im_v[...].reshape(seqs * groups, states)
    br, bi, fr, fi = map(per_seq, (bar_real, bar_imag, factor_real, factor_imag))
    new_real = br * sr - bi * si + (fr * drive_real - fi * drive_imag)
    new_imag = br * si + bi * sr + (fr * drive_imag + fi * drive_real)
    new_re_o[...] = new_real.reshape(seqs, groups, states)
    new_im_o[...] = new_imag.reshape(seqs, groups, states)
    out_re = out_re_v[...].reshape(channels, states).astype(BF16)
    out_im = out_im_v[...].reshape(channels, states).astype(BF16)
    full = lax.dot_general(
        new_real.astype(BF16), out_re, NT, preferred_element_type=F32
    ) - lax.dot_general(new_imag.astype(BF16), out_im, NT, preferred_element_type=F32)
    readout = jnp.concatenate(
        [
            jnp.sum(
                jnp.where(own, full[s * groups : (s + 1) * groups], 0.0), axis=0, keepdims=True
            )
            for s in range(seqs)
        ],
        axis=0,
    )
    readout = readout + skip_v[...] * projected
    activated = jax.nn.gelu(readout).astype(BF16)
    loads[13].wait()
    part_v[tp] = mm(activated, out_w_v[...]).astype(BF16)

    def part_copy(d):
        return pltpu.make_async_remote_copy(
            src_ref=part_v.at[tp],
            dst_ref=part_v.at[tp],
            send_sem=part_send.at[d],
            recv_sem=part_recv.at[tp],
            device_id={"tp": tp_peer(d)},
            device_id_type=MESH,
        )

    def part_arrival(d):
        p = tp_peer(d)
        return pltpu.make_async_remote_copy(
            src_ref=part_v.at[p],
            dst_ref=part_v.at[p],
            send_sem=part_send.at[d],
            recv_sem=part_recv.at[p],
            device_id={"tp": p},
            device_id_type=MESH,
        )

    pl.semaphore_wait(barrier, n_tp - 1 + n_ep - 1)
    for d in range(n_tp - 1, 0, -1):
        part_copy(d).start()

    base = ep * seqs
    by_row = route_masks(ids, base, seqs, slots, n_ep, span, True)
    by_lane = route_masks(ids, base, seqs, slots, n_ep, span, False)
    seq_lane, seq_row = iota((rows, seqs), 1), iota((seqs, rows), 0)
    select = jnp.zeros((rows, seqs), F32)
    table = jnp.zeros((seqs, rows), F32)
    for s in range(seqs):
        picked = functools.reduce(lambda a, b: a + b, by_row[s]).astype(F32)
        select = jnp.where(seq_lane == s, picked, select)
        weighed = functools.reduce(
            lambda a, b: a + b,
            [pick.astype(F32) * weights[s, k] for k, pick in enumerate(by_lane[s])],
        )
        table = jnp.where(seq_row == s, weighed, table)
    select = select.astype(BF16)

    loads[14].wait()
    for d in range(1, n_tp):
        part_arrival(d).wait_recv()
    delta = jnp.zeros((seqs, width), F32)
    for t in range(n_tp):
        delta = delta + part_v[t].astype(F32)
    hidden_state = (floats + delta).astype(BF16).astype(F32)
    hidden_v[...] = hidden_state
    normed = rms_scale(hidden_state, ffn_gain_v[...]).astype(BF16)
    xs_v[...] = mm(select, normed)
    for j in range(n_ep):
        outg_v[j] = xs_v[j * slots : (j + 1) * slots, :].astype(BF16)

    def swap(source, target, send, recv, d):
        return pltpu.make_async_remote_copy(
            src_ref=source.at[ep_to(d)],
            dst_ref=target.at[ep],
            send_sem=send.at[d],
            recv_sem=recv.at[ep],
            device_id={"ep": ep_to(d)},
            device_id_type=MESH,
        )

    def arrival(source, target, send, recv, d):
        j = ep_from(d)
        return pltpu.make_async_remote_copy(
            src_ref=source.at[j],
            dst_ref=target.at[j],
            send_sem=send.at[d],
            recv_sem=recv.at[j],
            device_id={"ep": j},
            device_id_type=MESH,
        )

    there = (outg_v, recvd_v, disp_send, disp_recv)
    back = (retg_v, retd_v, ret_send, ret_recv)
    for d in range(1, n_ep):
        swap(*there, d).start()
    recvd_v[ep] = outg_v[ep]
    for d in range(1, n_ep):
        arrival(*there, d).wait_recv()
    for j in range(n_ep):
        xs_v[j * slots : (j + 1) * slots, :] = recvd_v[j].astype(F32)
    x_v[...] = xs_v[...].astype(BF16)

    def hid_copy(c, d):
        return pltpu.make_async_remote_copy(
            src_ref=hid_v.at[tp, c],
            dst_ref=hid_v.at[tp, c],
            send_sem=hid_send.at[d, c],
            recv_sem=hid_recv.at[tp, c],
            device_id={"tp": tp_peer(d)},
            device_id_type=MESH,
        )

    def hid_arrival(c, d):
        p = tp_peer(d)
        return pltpu.make_async_remote_copy(
            src_ref=hid_v.at[p, c],
            dst_ref=hid_v.at[p, c],
            send_sem=hid_send.at[d, c],
            recv_sem=hid_recv.at[p, c],
            device_id={"tp": p},
            device_id_type=MESH,
        )

    def expand(c, _):
        for copy in gate_copy(c):
            copy.wait()
        x = x_v[...]
        gate_pre = mm(x, gate_v[c])
        up_pre = mm(x, up_v[c])
        hid_v[tp, c] = (jax.nn.silu(gate_pre) * up_pre).astype(BF16)
        for d in range(n_tp - 1, 0, -1):
            hid_copy(c, d).start()
        return 0

    lax.fori_loop(0, chunks, expand, 0)

    def contract(c, d):
        p = tp_peer(d)
        start = pl.multiple_of(p * piece + c * cw, cw)
        return mm(hid_v[p, c], down_v[pl.ds(start, cw), :])

    ys_v[...] = jnp.zeros_like(ys_v)
    for group in ([0], [1], list(range(2, n_tp))):
        for d in group:
            down_copy(tp_peer(d)).wait()

        def shrink(c, _, group=group):
            for d in group:
                if d > 0:
                    hid_arrival(c, d).wait_recv()
                ys_v[...] += contract(c, d)
            return 0

        lax.fori_loop(0, chunks, shrink, 0)

    for j in range(n_ep):
        retg_v[j] = ys_v[j * slots : (j + 1) * slots, :].astype(BF16)
    for d in range(1, n_ep):
        swap(*back, d).start()
    retd_v[ep] = retg_v[ep]
    for d in range(1, n_tp):
        part_copy(d).wait_send()
    for d in range(1, n_ep):
        swap(*there, d).wait_send()

    def sent(c, _):
        for d in range(1, n_tp):
            hid_copy(c, d).wait_send()
        return 0

    lax.fori_loop(0, chunks, sent, 0)
    residual = hidden_v[:, pl.ds(pl.multiple_of(tp * quarter, quarter), quarter)]
    for d in range(1, n_ep):
        arrival(*back, d).wait_recv()
    for j in range(n_ep):
        ys_v[j * slots : (j + 1) * slots, :] = retd_v[j].astype(F32)
    routed = jnp.dot(
        table, ys_v[...], preferred_element_type=F32, precision=lax.Precision.HIGHEST
    )
    mixed_o[...] = (residual + routed).astype(BF16)
    for d in range(1, n_ep):
        swap(*back, d).wait_send()


def shards(
    tokens,
    norm_gain,
    in_weight,
    decay_rate,
    frequency,
    log_step,
    input_real,
    input_imag,
    output_real,
    output_imag,
    skip_gain,
    state_real,
    state_imag,
    out_weight,
    ffn_gain,
    expert_ids,
    route_weights,
    gate_weight,
    up_weight,
    down_weight,
):
    n_ep, n_tp = lax.axis_size("ep"), lax.axis_size("tp")
    seqs, width = tokens.shape
    slots = seqs // 2
    rows = n_ep * slots
    columns = gate_weight.shape[1]
    cw = min(512, columns)
    chunks = columns // cw
    quarter = down_weight.shape[1]
    groups, states, chan = input_real.shape
    operands = [
        tokens,
        norm_gain.reshape(1, -1),
        in_weight,
        decay_rate,
        frequency,
        log_step.reshape(1, -1),
        input_real,
        input_imag,
        output_real,
        output_imag,
        skip_gain.reshape(1, -1),
        state_real,
        state_imag,
        out_weight,
        ffn_gain.reshape(1, -1),
        expert_ids,
        route_weights,
        gate_weight,
        up_weight,
        down_weight,
    ]
    any_spec = pl.BlockSpec(memory_space=pl.ANY)
    smem = pl.BlockSpec(memory_space=pltpu.SMEM)
    vmem = pl.BlockSpec(memory_space=pltpu.VMEM)
    dma = pltpu.SemaphoreType.DMA
    copies = [pltpu.VMEM(value.shape, value.dtype) for value in operands[:15]]
    return pl.pallas_call(
        functools.partial(kernel, n_ep, n_tp),
        out_shape=(
            jax.ShapeDtypeStruct((seqs, quarter), BF16),
            jax.ShapeDtypeStruct(state_real.shape, F32),
            jax.ShapeDtypeStruct(state_imag.shape, F32),
        ),
        in_specs=[any_spec] * 15 + [smem] * 2 + [any_spec] * 3,
        out_specs=(vmem, vmem, vmem),
        scratch_shapes=copies
        + [
            pltpu.VMEM((chunks, width, cw), BF16),
            pltpu.VMEM((chunks, width, cw), BF16),
            pltpu.VMEM(down_weight.shape, BF16),
            pltpu.VMEM((groups, chan, 2 * states), BF16),
            pltpu.VMEM((n_tp, seqs, width), BF16),
            pltpu.VMEM((seqs, width), F32),
            pltpu.VMEM((rows, width), F32),
            pltpu.VMEM((rows, width), BF16),
            pltpu.VMEM((n_ep, slots, width), BF16),
            pltpu.VMEM((n_ep, slots, width), BF16),
            pltpu.VMEM((n_tp, chunks, rows, cw), BF16),
            pltpu.VMEM((rows, quarter), F32),
            pltpu.VMEM((n_ep, slots, quarter), BF16),
            pltpu.VMEM((n_ep, slots, quarter), BF16),
            dma((15,)),
            dma((chunks,)),
            dma((chunks,)),
            dma((n_tp,)),
            dma((n_tp,)),
            dma((n_tp,)),
            dma((n_ep,)),
            dma((n_ep,)),
            dma((n_tp, chunks)),
            dma((n_tp, chunks)),
            dma((n_ep,)),
            dma((n_ep,)),
        ],
        compiler_params=pltpu.CompilerParams(
            collective_id=0, has_side_effects=True, vmem_limit_bytes=60 * 1024 * 1024
        ),
        name="layer",
    )(*operands)


def solution(mesh):
    in_specs = (
        P("ep", None),
        P(),
        P(None, "tp"),
        P("tp", None),
        P("tp", None),
        P("tp"),
        P("tp", None, None),
        P("tp", None, None),
        P("tp", None, None),
        P("tp", None, None),
        P("tp"),
        P("ep", "tp", None),
        P("ep", "tp", None),
        P("tp", None),
        P(),
        P(),
        P("ep", None),
        P(None, ("ep", "tp")),
        P(None, ("ep", "tp")),
        P("ep", "tp"),
    )
    out_specs = (P("ep", "tp"), P("ep", "tp", None), P("ep", "tp", None))
    return jax.shard_map(shards, mesh=mesh, in_specs=in_specs, out_specs=out_specs, check_vma=False)
```

```python
import functools

import jax
import jax.numpy as jnp
from jax import lax
from jax.experimental import pallas as pl
from jax.experimental.pallas import tpu as pltpu
from jax.sharding import PartitionSpec as P

EXPERTS = 8
EPSILON = 1e-06
MESH = pl.DeviceIdType.MESH
F32, BF16 = jnp.float32, jnp.bfloat16
NT = (((1,), (1,)), ((), ()))


def rms_scale(floats, gain):
    return (
        floats
        * lax.rsqrt(jnp.mean(floats * floats, axis=-1, keepdims=True) + EPSILON)
        * gain
    )


def flat_row(ref):
    values = ref[...].astype(F32)
    return jnp.concatenate([values[i : i + 1] for i in range(values.shape[0])], axis=1)


def mm(a, b):
    return jnp.dot(a, b, preferred_element_type=F32)


def iota(shape, axis):
    return lax.broadcasted_iota(jnp.int32, shape, axis)


def route_masks(ids, base, seqs, slots, owners, span, rows_first):
    shape = (owners * slots, 1) if rows_first else (1, owners * slots)
    place = iota(shape, 0 if rows_first else 1)
    expert, slot = place // (slots * span), place % slots
    count = jnp.zeros(shape, jnp.int32)
    masks = []
    for s in range(seqs):
        picks = []
        hit = jnp.zeros(shape, jnp.int32)
        for k in range(ids.shape[0]):
            same = jnp.where(expert == ids[k, base + s], 1, 0)
            picks.append(jnp.where(count == slot, same, 0))
            hit = hit + same
        masks.append(picks)
        count = count + hit
    return masks


def kernel(
    n_ep,
    n_tp,
    tokens_h,
    norm_gain_h,
    in_w_h,
    decay_h,
    freq_h,
    log_step_h,
    in_re_h,
    in_im_h,
    out_re_h,
    out_im_h,
    skip_h,
    st_re_h,
    st_im_h,
    out_w_h,
    ffn_gain_h,
    ids,
    weights,
    gate_h,
    up_h,
    down_h,
    mixed_o,
    new_re_o,
    new_im_o,
    tokens_v,
    norm_gain_v,
    in_w_v,
    decay_v,
    freq_v,
    log_step_v,
    in_re_v,
    in_im_v,
    out_re_v,
    out_im_v,
    skip_v,
    st_re_v,
    st_im_v,
    out_w_v,
    ffn_gain_v,
    gate_v,
    up_v,
    down_v,
    part_v,
    hidden_v,
    xs_v,
    x_v,
    outg_v,
    recvd_v,
    hid_v,
    ys_v,
    retg_v,
    retd_v,
    load_sem,
    gate_sem,
    up_sem,
    down_sem,
    part_send,
    part_recv,
    disp_send,
    disp_recv,
    hid_send,
    hid_recv,
    ret_send,
    ret_recv,
):
    ep, tp = lax.axis_index("ep"), lax.axis_index("tp")
    chunks, _, cw = gate_v.shape
    seqs, width = tokens_v.shape
    groups, states = decay_v.shape
    chan = in_re_v.shape[1]
    slots = seqs // 2
    span = n_ep // EXPERTS
    rows = n_ep * slots
    quarter = down_v.shape[1]
    piece = chunks * cw

    def tp_peer(d):
        return (tp // 2 * 2 + d // 2 * 2) % n_tp + (tp % 2 + d % 2) % 2

    def ep_to(d):
        return (ep + d) % n_ep

    def ep_from(d):
        return (ep + n_ep - d) % n_ep

    pairs = [
        (tokens_h, tokens_v),
        (norm_gain_h, norm_gain_v),
        (in_w_h, in_w_v),
        (in_re_h, in_re_v),
        (in_im_h, in_im_v),
        (log_step_h, log_step_v),
        (decay_h, decay_v),
        (freq_h, freq_v),
        (st_re_h, st_re_v),
        (st_im_h, st_im_v),
        (out_re_h, out_re_v),
        (out_im_h, out_im_v),
        (skip_h, skip_v),
        (out_w_h, out_w_v),
        (ffn_gain_h, ffn_gain_v),
    ]
    loads = [pltpu.make_async_copy(a, b, load_sem.at[i]) for i, (a, b) in enumerate(pairs)]
    for load in loads:
        load.start()

    barrier = pltpu.get_barrier_semaphore()
    for d in range(1, n_tp):
        pl.semaphore_signal(barrier, inc=1, device_id={"tp": tp_peer(d)}, device_id_type=MESH)
    for d in range(1, n_ep):
        pl.semaphore_signal(barrier, inc=1, device_id={"ep": ep_to(d)}, device_id_type=MESH)

    def gate_copy(c):
        cols = pl.ds(pl.multiple_of(c * cw, cw), cw)
        return (
            pltpu.make_async_copy(gate_h.at[:, cols], gate_v.at[c], gate_sem.at[c]),
            pltpu.make_async_copy(up_h.at[:, cols], up_v.at[c], up_sem.at[c]),
        )

    def down_copy(p):
        part = pl.ds(pl.multiple_of(p * piece, piece), piece)
        return pltpu.make_async_copy(down_h.at[part], down_v.at[part], down_sem.at[p])

    for c in range(chunks):
        for copy in gate_copy(c):
            copy.start()
    for d in range(n_tp):
        down_copy(tp_peer(d)).start()

    for load in loads[3:8]:
        load.wait()
    eye = iota((groups, groups), 0) == iota((groups, groups), 1)
    step_size = jnp.sum(jnp.where(eye, jnp.exp(log_step_v[...]), 0.0), axis=1, keepdims=True)
    lam_real, frequency = -decay_v[...], freq_v[...]
    magnitude = jnp.exp(lam_real * step_size)
    turned = frequency * step_size
    bar_real = magnitude * jnp.cos(turned)
    bar_imag = magnitude * jnp.sin(turned)
    denom = lam_real * lam_real + frequency * frequency
    minus_one = bar_real - 1.0
    factor_real = (minus_one * lam_real + bar_imag * frequency) / denom
    factor_imag = (bar_imag * lam_real - minus_one * frequency) / denom

    def per_seq(values):
        return jnp.concatenate([values] * seqs, axis=0)

    for load in loads[0:3]:
        load.wait()
    floats = tokens_v[...].astype(F32)
    normed_in = rms_scale(floats, flat_row(norm_gain_v)).astype(BF16)
    projected = mm(normed_in, in_w_v[...]).astype(BF16).astype(F32)
    channels = projected.shape[1]
    own = iota((groups, channels), 1) // chan == iota((groups, channels), 0)
    spread = jnp.concatenate(
        [
            jnp.where(own, jnp.broadcast_to(projected[s : s + 1], own.shape), 0.0)
            for s in range(seqs)
        ],
        axis=0,
    ).astype(BF16)
    drive_real = mm(spread, in_re_v[...].reshape(channels, states).astype(BF16))
    drive_imag = mm(spread, in_im_v[...].reshape(channels, states).astype(BF16))
    for load in loads[8:13]:
        load.wait()
    sr = st_re_v[...].reshape(seqs * groups, states)
    si = st_im_v[...].reshape(seqs * groups, states)
    br, bi, fr, fi = map(per_seq, (bar_real, bar_imag, factor_real, factor_imag))
    new_real = br * sr - bi * si + (fr * drive_real - fi * drive_imag)
    new_imag = br * si + bi * sr + (fr * drive_imag + fi * drive_real)
    new_re_o[...] = new_real.reshape(seqs, groups, states)
    new_im_o[...] = new_imag.reshape(seqs, groups, states)
    out_re = out_re_v[...].reshape(channels, states).astype(BF16)
    out_im = out_im_v[...].reshape(channels, states).astype(BF16)
    full = lax.dot_general(
        new_real.astype(BF16), out_re, NT, preferred_element_type=F32
    ) - lax.dot_general(new_imag.astype(BF16), out_im, NT, preferred_element_type=F32)
    readout = jnp.concatenate(
        [
            jnp.sum(
                jnp.where(own, full[s * groups : (s + 1) * groups], 0.0), axis=0, keepdims=True
            )
            for s in range(seqs)
        ],
        axis=0,
    )
    readout = readout + skip_v[...] * projected
    activated = jax.nn.gelu(readout).astype(BF16)
    loads[13].wait()
    part_v[tp] = mm(activated, out_w_v[...]).astype(BF16)

    def part_copy(d):
        return pltpu.make_async_remote_copy(
            src_ref=part_v.at[tp],
            dst_ref=part_v.at[tp],
            send_sem=part_send.at[d],
            recv_sem=part_recv.at[tp],
            device_id={"tp": tp_peer(d)},
            device_id_type=MESH,
        )

    def part_arrival(d):
        p = tp_peer(d)
        return pltpu.make_async_remote_copy(
            src_ref=part_v.at[p],
            dst_ref=part_v.at[p],
            send_sem=part_send.at[d],
            recv_sem=part_recv.at[p],
            device_id={"tp": p},
            device_id_type=MESH,
        )

    pl.semaphore_wait(barrier, n_tp - 1 + n_ep - 1)
    for d in range(n_tp - 1, 0, -1):
        part_copy(d).start()

    base = ep * seqs
    by_row = route_masks(ids, base, seqs, slots, n_ep, span, True)
    by_lane = route_masks(ids, base, seqs, slots, n_ep, span, False)
    seq_lane, seq_row = iota((rows, seqs), 1), iota((seqs, rows), 0)
    select = jnp.zeros((rows, seqs), F32)
    table = jnp.zeros((seqs, rows), F32)
    for s in range(seqs):
        picked = functools.reduce(lambda a, b: a + b, by_row[s]).astype(F32)
        select = jnp.where(seq_lane == s, picked, select)
        weighed = functools.reduce(
            lambda a, b: a + b,
            [pick.astype(F32) * weights[k, s] for k, pick in enumerate(by_lane[s])],
        )
        table = jnp.where(seq_row == s, weighed, table)
    select = select.astype(BF16)

    loads[14].wait()
    ffn_gain = flat_row(ffn_gain_v)
    for d in range(1, n_tp):
        part_arrival(d).wait_recv()
    delta = jnp.zeros((seqs, width), F32)
    for t in range(n_tp):
        delta = delta + part_v[t].astype(F32)
    hidden_state = (floats + delta).astype(BF16).astype(F32)
    hidden_v[...] = hidden_state
    normed = rms_scale(hidden_state, ffn_gain).astype(BF16)
    xs_v[...] = mm(select, normed)
    for j in range(n_ep):
        outg_v[j] = xs_v[j * slots : (j + 1) * slots, :].astype(BF16)

    def swap(source, target, send, recv, d):
        return pltpu.make_async_remote_copy(
            src_ref=source.at[ep_to(d)],
            dst_ref=target.at[ep],
            send_sem=send.at[d],
            recv_sem=recv.at[ep],
            device_id={"ep": ep_to(d)},
            device_id_type=MESH,
        )

    def arrival(source, target, send, recv, d):
        j = ep_from(d)
        return pltpu.make_async_remote_copy(
            src_ref=source.at[j],
            dst_ref=target.at[j],
            send_sem=send.at[d],
            recv_sem=recv.at[j],
            device_id={"ep": j},
            device_id_type=MESH,
        )

    there = (outg_v, recvd_v, disp_send, disp_recv)
    back = (retg_v, retd_v, ret_send, ret_recv)
    for d in range(1, n_ep):
        swap(*there, d).start()
    recvd_v[ep] = outg_v[ep]
    for d in range(1, n_ep):
        arrival(*there, d).wait_recv()
    for j in range(n_ep):
        xs_v[j * slots : (j + 1) * slots, :] = recvd_v[j].astype(F32)
    x_v[...] = xs_v[...].astype(BF16)

    def hid_copy(c, d):
        return pltpu.make_async_remote_copy(
            src_ref=hid_v.at[tp, c],
            dst_ref=hid_v.at[tp, c],
            send_sem=hid_send.at[d, c],
            recv_sem=hid_recv.at[tp, c],
            device_id={"tp": tp_peer(d)},
            device_id_type=MESH,
        )

    def hid_arrival(c, d):
        p = tp_peer(d)
        return pltpu.make_async_remote_copy(
            src_ref=hid_v.at[p, c],
            dst_ref=hid_v.at[p, c],
            send_sem=hid_send.at[d, c],
            recv_sem=hid_recv.at[p, c],
            device_id={"tp": p},
            device_id_type=MESH,
        )

    def expand(c, _):
        for copy in gate_copy(c):
            copy.wait()
        x = x_v[...]
        gate_pre = mm(x, gate_v[c])
        up_pre = mm(x, up_v[c])
        hid_v[tp, c] = (jax.nn.silu(gate_pre) * up_pre).astype(BF16)
        for d in range(n_tp - 1, 0, -1):
            hid_copy(c, d).start()
        return 0

    lax.fori_loop(0, chunks, expand, 0)

    def contract(c, d):
        p = tp_peer(d)
        start = pl.multiple_of(p * piece + c * cw, cw)
        return mm(hid_v[p, c], down_v[pl.ds(start, cw), :])

    ys_v[...] = jnp.zeros_like(ys_v)
    for group in ([0], [1], list(range(2, n_tp))):
        for d in group:
            down_copy(tp_peer(d)).wait()

        def shrink(c, _, group=group):
            for d in group:
                if d > 0:
                    hid_arrival(c, d).wait_recv()
                ys_v[...] += contract(c, d)
            return 0

        lax.fori_loop(0, chunks, shrink, 0)

    for j in range(n_ep):
        retg_v[j] = ys_v[j * slots : (j + 1) * slots, :].astype(BF16)
    for d in range(1, n_ep):
        swap(*back, d).start()
    retd_v[ep] = retg_v[ep]
    for d in range(1, n_tp):
        part_copy(d).wait_send()
    for d in range(1, n_ep):
        swap(*there, d).wait_send()

    def sent(c, _):
        for d in range(1, n_tp):
            hid_copy(c, d).wait_send()
        return 0

    lax.fori_loop(0, chunks, sent, 0)
    residual = hidden_v[:, pl.ds(pl.multiple_of(tp * quarter, quarter), quarter)]
    for d in range(1, n_ep):
        arrival(*back, d).wait_recv()
    for j in range(n_ep):
        ys_v[j * slots : (j + 1) * slots, :] = retd_v[j].astype(F32)
    routed = jnp.dot(
        table, ys_v[...], preferred_element_type=F32, precision=lax.Precision.HIGHEST
    )
    mixed_o[...] = (residual + routed).astype(BF16)
    for d in range(1, n_ep):
        swap(*back, d).wait_send()


def hand_over(*refs):
    for source, target in zip(refs[:3], refs[3:]):
        target[...] = source[...]


def shards(
    tokens,
    norm_gain,
    in_weight,
    decay_rate,
    frequency,
    log_step,
    input_real,
    input_imag,
    output_real,
    output_imag,
    skip_gain,
    state_real,
    state_imag,
    out_weight,
    ffn_gain,
    expert_ids,
    route_weights,
    gate_weight,
    up_weight,
    down_weight,
):
    n_ep, n_tp = lax.axis_size("ep"), lax.axis_size("tp")
    seqs, width = tokens.shape
    slots = seqs // 2
    rows = n_ep * slots
    columns = gate_weight.shape[1]
    cw = min(512, columns)
    chunks = columns // cw
    quarter = down_weight.shape[1]
    operands = [
        tokens,
        norm_gain.reshape(-1, 128),
        in_weight,
        decay_rate,
        frequency,
        log_step.reshape(1, -1),
        jnp.swapaxes(input_real, 1, 2),
        jnp.swapaxes(input_imag, 1, 2),
        output_real,
        output_imag,
        skip_gain.reshape(1, -1),
        state_real,
        state_imag,
        out_weight,
        ffn_gain.reshape(-1, 128),
        expert_ids.T,
        route_weights.T,
        gate_weight,
        up_weight,
        down_weight,
    ]
    any_spec = pl.BlockSpec(memory_space=pl.ANY)
    smem = pl.BlockSpec(memory_space=pltpu.SMEM)
    vmem = pl.BlockSpec(memory_space=pltpu.VMEM)
    dma = pltpu.SemaphoreType.DMA
    copies = [pltpu.VMEM(value.shape, value.dtype) for value in operands[:15]]
    results = pl.pallas_call(
        functools.partial(kernel, n_ep, n_tp),
        out_shape=(
            jax.ShapeDtypeStruct((seqs, quarter), BF16),
            jax.ShapeDtypeStruct(state_real.shape, F32),
            jax.ShapeDtypeStruct(state_imag.shape, F32),
        ),
        in_specs=[any_spec] * 15 + [smem] * 2 + [any_spec] * 3,
        out_specs=(vmem, vmem, vmem),
        scratch_shapes=copies
        + [
            pltpu.VMEM((chunks, width, cw), BF16),
            pltpu.VMEM((chunks, width, cw), BF16),
            pltpu.VMEM(down_weight.shape, BF16),
            pltpu.VMEM((n_tp, seqs, width), BF16),
            pltpu.VMEM((seqs, width), F32),
            pltpu.VMEM((rows, width), F32),
            pltpu.VMEM((rows, width), BF16),
            pltpu.VMEM((n_ep, slots, width), BF16),
            pltpu.VMEM((n_ep, slots, width), BF16),
            pltpu.VMEM((n_tp, chunks, rows, cw), BF16),
            pltpu.VMEM((rows, quarter), F32),
            pltpu.VMEM((n_ep, slots, quarter), BF16),
            pltpu.VMEM((n_ep, slots, quarter), BF16),
            dma((15,)),
            dma((chunks,)),
            dma((chunks,)),
            dma((n_tp,)),
            dma((n_tp,)),
            dma((n_tp,)),
            dma((n_ep,)),
            dma((n_ep,)),
            dma((n_tp, chunks)),
            dma((n_tp, chunks)),
            dma((n_ep,)),
            dma((n_ep,)),
        ],
        compiler_params=pltpu.CompilerParams(
            collective_id=0, has_side_effects=True, vmem_limit_bytes=60 * 1024 * 1024
        ),
        name="layer",
    )(*operands)
    return pl.pallas_call(
        hand_over,
        out_shape=tuple(jax.ShapeDtypeStruct(r.shape, r.dtype) for r in results),
        in_specs=[vmem] * 3,
        out_specs=(vmem,) * 3,
        name="hand_over",
    )(*results)


def solution(mesh):
    in_specs = (
        P("ep", None),
        P(),
        P(None, "tp"),
        P("tp", None),
        P("tp", None),
        P("tp"),
        P("tp", None, None),
        P("tp", None, None),
        P("tp", None, None),
        P("tp", None, None),
        P("tp"),
        P("ep", "tp", None),
        P("ep", "tp", None),
        P("tp", None),
        P(),
        P(),
        P("ep", None),
        P(None, ("ep", "tp")),
        P(None, ("ep", "tp")),
        P("ep", "tp"),
    )
    out_specs = (P("ep", "tp"), P("ep", "tp", None), P("ep", "tp", None))
    return jax.shard_map(shards, mesh=mesh, in_specs=in_specs, out_specs=out_specs, check_vma=False)
```

```python
import functools

import jax
import jax.numpy as jnp
from jax import lax
from jax.experimental import pallas as pl
from jax.experimental.pallas import tpu as pltpu
from jax.sharding import PartitionSpec as P

EXPERTS = 8
EPSILON = 1e-06
MESH = pl.DeviceIdType.MESH
F32, BF16 = jnp.float32, jnp.bfloat16
NT = (((1,), (1,)), ((), ()))


def rms_scale(floats, gain):
    return (
        floats
        * lax.rsqrt(jnp.mean(floats * floats, axis=-1, keepdims=True) + EPSILON)
        * gain
    )


def flat_row(ref):
    values = ref[...].astype(F32)
    return jnp.concatenate([values[i : i + 1] for i in range(values.shape[0])], axis=1)


def mm(a, b):
    return jnp.dot(a, b, preferred_element_type=F32)


def iota(shape, axis):
    return lax.broadcasted_iota(jnp.int32, shape, axis)


def route_masks(ids, base, seqs, slots, owners, span, rows_first):
    shape = (owners * slots, 1) if rows_first else (1, owners * slots)
    place = iota(shape, 0 if rows_first else 1)
    expert, slot = place // (slots * span), place % slots
    count = jnp.zeros(shape, jnp.int32)
    masks = []
    for s in range(seqs):
        picks = []
        hit = jnp.zeros(shape, jnp.int32)
        for k in range(ids.shape[0]):
            same = jnp.where(expert == ids[k, base + s], 1, 0)
            picks.append(jnp.where(count == slot, same, 0))
            hit = hit + same
        masks.append(picks)
        count = count + hit
    return masks


def kernel(
    n_ep,
    n_tp,
    tokens_h,
    norm_gain_h,
    in_w_h,
    decay_h,
    freq_h,
    log_step_h,
    in_re_h,
    in_im_h,
    out_re_h,
    out_im_h,
    skip_h,
    st_re_h,
    st_im_h,
    out_w_h,
    ffn_gain_h,
    ids,
    weights,
    gate_h,
    up_h,
    down_h,
    mixed_o,
    new_re_o,
    new_im_o,
    tokens_v,
    norm_gain_v,
    in_w_v,
    decay_v,
    freq_v,
    log_step_v,
    in_re_v,
    in_im_v,
    out_re_v,
    out_im_v,
    skip_v,
    st_re_v,
    st_im_v,
    out_w_v,
    ffn_gain_v,
    gate_v,
    up_v,
    down_v,
    part_v,
    hidden_v,
    xs_v,
    x_v,
    outg_v,
    recvd_v,
    hid_v,
    ys_v,
    retg_v,
    retd_v,
    load_sem,
    gate_sem,
    up_sem,
    down_sem,
    part_send,
    part_recv,
    disp_send,
    disp_recv,
    hid_send,
    hid_recv,
    ret_send,
    ret_recv,
):
    ep, tp = lax.axis_index("ep"), lax.axis_index("tp")
    chunks, _, cw = gate_v.shape
    seqs, width = tokens_v.shape
    groups, states = decay_v.shape
    chan = in_re_v.shape[1]
    slots = seqs // 2
    span = n_ep // EXPERTS
    rows = n_ep * slots
    quarter = down_v.shape[1]
    piece = chunks * cw

    def tp_peer(d):
        return (tp // 2 * 2 + d // 2 * 2) % n_tp + (tp % 2 + d % 2) % 2

    def ep_to(d):
        return (ep + d) % n_ep

    def ep_from(d):
        return (ep + n_ep - d) % n_ep

    pairs = [
        (tokens_h, tokens_v),
        (norm_gain_h, norm_gain_v),
        (in_w_h, in_w_v),
        (in_re_h, in_re_v),
        (in_im_h, in_im_v),
        (log_step_h, log_step_v),
        (decay_h, decay_v),
        (freq_h, freq_v),
        (st_re_h, st_re_v),
        (st_im_h, st_im_v),
        (out_re_h, out_re_v),
        (out_im_h, out_im_v),
        (skip_h, skip_v),
        (out_w_h, out_w_v),
        (ffn_gain_h, ffn_gain_v),
    ]
    loads = [pltpu.make_async_copy(a, b, load_sem.at[i]) for i, (a, b) in enumerate(pairs)]
    for load in loads:
        load.start()

    barrier = pltpu.get_barrier_semaphore()
    for d in range(1, n_tp):
        pl.semaphore_signal(barrier, inc=1, device_id={"tp": tp_peer(d)}, device_id_type=MESH)
    for d in range(1, n_ep):
        pl.semaphore_signal(barrier, inc=1, device_id={"ep": ep_to(d)}, device_id_type=MESH)

    def gate_copy(c):
        cols = pl.ds(pl.multiple_of(c * cw, cw), cw)
        return (
            pltpu.make_async_copy(gate_h.at[:, cols], gate_v.at[c], gate_sem.at[c]),
            pltpu.make_async_copy(up_h.at[:, cols], up_v.at[c], up_sem.at[c]),
        )

    def down_copy(p):
        part = pl.ds(pl.multiple_of(p * piece, piece), piece)
        return pltpu.make_async_copy(down_h.at[part], down_v.at[part], down_sem.at[p])

    for load in loads[3:8]:
        load.wait()
    eye = iota((groups, groups), 0) == iota((groups, groups), 1)
    step_size = jnp.sum(jnp.where(eye, jnp.exp(log_step_v[...]), 0.0), axis=1, keepdims=True)
    lam_real, frequency = -decay_v[...], freq_v[...]
    magnitude = jnp.exp(lam_real * step_size)
    turned = frequency * step_size
    bar_real = magnitude * jnp.cos(turned)
    bar_imag = magnitude * jnp.sin(turned)
    denom = lam_real * lam_real + frequency * frequency
    minus_one = bar_real - 1.0
    factor_real = (minus_one * lam_real + bar_imag * frequency) / denom
    factor_imag = (bar_imag * lam_real - minus_one * frequency) / denom

    def per_seq(values):
        return jnp.concatenate([values] * seqs, axis=0)

    for load in loads[0:3]:
        load.wait()
    for c in range(chunks):
        for copy in gate_copy(c):
            copy.start()
    for d in range(n_tp):
        down_copy(tp_peer(d)).start()
    floats = tokens_v[...].astype(F32)
    normed_in = rms_scale(floats, flat_row(norm_gain_v)).astype(BF16)
    projected = mm(normed_in, in_w_v[...]).astype(BF16).astype(F32)
    channels = projected.shape[1]
    own = iota((groups, channels), 1) // chan == iota((groups, channels), 0)
    spread = jnp.concatenate(
        [
            jnp.where(own, jnp.broadcast_to(projected[s : s + 1], own.shape), 0.0)
            for s in range(seqs)
        ],
        axis=0,
    ).astype(BF16)
    drive_real = mm(spread, in_re_v[...].reshape(channels, states).astype(BF16))
    drive_imag = mm(spread, in_im_v[...].reshape(channels, states).astype(BF16))
    for load in loads[8:13]:
        load.wait()
    sr = st_re_v[...].reshape(seqs * groups, states)
    si = st_im_v[...].reshape(seqs * groups, states)
    br, bi, fr, fi = map(per_seq, (bar_real, bar_imag, factor_real, factor_imag))
    new_real = br * sr - bi * si + (fr * drive_real - fi * drive_imag)
    new_imag = br * si + bi * sr + (fr * drive_imag + fi * drive_real)
    new_re_o[...] = new_real.reshape(seqs, groups, states)
    new_im_o[...] = new_imag.reshape(seqs, groups, states)
    out_re = out_re_v[...].reshape(channels, states).astype(BF16)
    out_im = out_im_v[...].reshape(channels, states).astype(BF16)
    full = lax.dot_general(
        new_real.astype(BF16), out_re, NT, preferred_element_type=F32
    ) - lax.dot_general(new_imag.astype(BF16), out_im, NT, preferred_element_type=F32)
    readout = jnp.concatenate(
        [
            jnp.sum(
                jnp.where(own, full[s * groups : (s + 1) * groups], 0.0), axis=0, keepdims=True
            )
            for s in range(seqs)
        ],
        axis=0,
    )
    readout = readout + skip_v[...] * projected
    activated = jax.nn.gelu(readout).astype(BF16)
    loads[13].wait()
    part_v[tp] = mm(activated, out_w_v[...]).astype(BF16)

    def part_copy(d):
        return pltpu.make_async_remote_copy(
            src_ref=part_v.at[tp],
            dst_ref=part_v.at[tp],
            send_sem=part_send.at[d],
            recv_sem=part_recv.at[tp],
            device_id={"tp": tp_peer(d)},
            device_id_type=MESH,
        )

    def part_arrival(d):
        p = tp_peer(d)
        return pltpu.make_async_remote_copy(
            src_ref=part_v.at[p],
            dst_ref=part_v.at[p],
            send_sem=part_send.at[d],
            recv_sem=part_recv.at[p],
            device_id={"tp": p},
            device_id_type=MESH,
        )

    pl.semaphore_wait(barrier, n_tp - 1 + n_ep - 1)
    for d in range(n_tp - 1, 0, -1):
        part_copy(d).start()

    base = ep * seqs
    by_row = route_masks(ids, base, seqs, slots, n_ep, span, True)
    by_lane = route_masks(ids, base, seqs, slots, n_ep, span, False)
    seq_lane, seq_row = iota((rows, seqs), 1), iota((seqs, rows), 0)
    select = jnp.zeros((rows, seqs), F32)
    table = jnp.zeros((seqs, rows), F32)
    for s in range(seqs):
        picked = functools.reduce(lambda a, b: a + b, by_row[s]).astype(F32)
        select = jnp.where(seq_lane == s, picked, select)
        weighed = functools.reduce(
            lambda a, b: a + b,
            [pick.astype(F32) * weights[k, s] for k, pick in enumerate(by_lane[s])],
        )
        table = jnp.where(seq_row == s, weighed, table)
    select = select.astype(BF16)

    loads[14].wait()
    ffn_gain = flat_row(ffn_gain_v)
    for d in range(1, n_tp):
        part_arrival(d).wait_recv()
    delta = jnp.zeros((seqs, width), F32)
    for t in range(n_tp):
        delta = delta + part_v[t].astype(F32)
    hidden_state = (floats + delta).astype(BF16).astype(F32)
    hidden_v[...] = hidden_state
    normed = rms_scale(hidden_state, ffn_gain).astype(BF16)
    xs_v[...] = mm(select, normed)
    for j in range(n_ep):
        outg_v[j] = xs_v[j * slots : (j + 1) * slots, :].astype(BF16)

    def swap(source, target, send, recv, d):
        return pltpu.make_async_remote_copy(
            src_ref=source.at[ep_to(d)],
            dst_ref=target.at[ep],
            send_sem=send.at[d],
            recv_sem=recv.at[ep],
            device_id={"ep": ep_to(d)},
            device_id_type=MESH,
        )

    def arrival(source, target, send, recv, d):
        j = ep_from(d)
        return pltpu.make_async_remote_copy(
            src_ref=source.at[j],
            dst_ref=target.at[j],
            send_sem=send.at[d],
            recv_sem=recv.at[j],
            device_id={"ep": j},
            device_id_type=MESH,
        )

    there = (outg_v, recvd_v, disp_send, disp_recv)
    back = (retg_v, retd_v, ret_send, ret_recv)
    for d in range(1, n_ep):
        swap(*there, d).start()
    recvd_v[ep] = outg_v[ep]
    for d in range(1, n_ep):
        arrival(*there, d).wait_recv()
    for j in range(n_ep):
        xs_v[j * slots : (j + 1) * slots, :] = recvd_v[j].astype(F32)
    x_v[...] = xs_v[...].astype(BF16)

    def hid_copy(c, d):
        return pltpu.make_async_remote_copy(
            src_ref=hid_v.at[tp, c],
            dst_ref=hid_v.at[tp, c],
            send_sem=hid_send.at[d, c],
            recv_sem=hid_recv.at[tp, c],
            device_id={"tp": tp_peer(d)},
            device_id_type=MESH,
        )

    def hid_arrival(c, d):
        p = tp_peer(d)
        return pltpu.make_async_remote_copy(
            src_ref=hid_v.at[p, c],
            dst_ref=hid_v.at[p, c],
            send_sem=hid_send.at[d, c],
            recv_sem=hid_recv.at[p, c],
            device_id={"tp": p},
            device_id_type=MESH,
        )

    def expand(c, _):
        for copy in gate_copy(c):
            copy.wait()
        x = x_v[...]
        gate_pre = mm(x, gate_v[c])
        up_pre = mm(x, up_v[c])
        hid_v[tp, c] = (jax.nn.silu(gate_pre) * up_pre).astype(BF16)
        for d in range(n_tp - 1, 0, -1):
            hid_copy(c, d).start()
        return 0

    lax.fori_loop(0, chunks, expand, 0)

    def contract(c, d):
        p = tp_peer(d)
        start = pl.multiple_of(p * piece + c * cw, cw)
        return mm(hid_v[p, c], down_v[pl.ds(start, cw), :])

    ys_v[...] = jnp.zeros_like(ys_v)
    for group in ([0], [1], list(range(2, n_tp))):
        for d in group:
            down_copy(tp_peer(d)).wait()

        def shrink(c, _, group=group):
            for d in group:
                if d > 0:
                    hid_arrival(c, d).wait_recv()
                ys_v[...] += contract(c, d)
            return 0

        lax.fori_loop(0, chunks, shrink, 0)

    for j in range(n_ep):
        retg_v[j] = ys_v[j * slots : (j + 1) * slots, :].astype(BF16)
    for d in range(1, n_ep):
        swap(*back, d).start()
    retd_v[ep] = retg_v[ep]
    for d in range(1, n_tp):
        part_copy(d).wait_send()
    for d in range(1, n_ep):
        swap(*there, d).wait_send()

    def sent(c, _):
        for d in range(1, n_tp):
            hid_copy(c, d).wait_send()
        return 0

    lax.fori_loop(0, chunks, sent, 0)
    residual = hidden_v[:, pl.ds(pl.multiple_of(tp * quarter, quarter), quarter)]
    for d in range(1, n_ep):
        arrival(*back, d).wait_recv()
    for j in range(n_ep):
        ys_v[j * slots : (j + 1) * slots, :] = retd_v[j].astype(F32)
    routed = jnp.dot(
        table, ys_v[...], preferred_element_type=F32, precision=lax.Precision.HIGHEST
    )
    mixed_o[...] = (residual + routed).astype(BF16)
    for d in range(1, n_ep):
        swap(*back, d).wait_send()


def hand_over(*refs):
    for source, target in zip(refs[:3], refs[3:]):
        target[...] = source[...]


def shards(
    tokens,
    norm_gain,
    in_weight,
    decay_rate,
    frequency,
    log_step,
    input_real,
    input_imag,
    output_real,
    output_imag,
    skip_gain,
    state_real,
    state_imag,
    out_weight,
    ffn_gain,
    expert_ids,
    route_weights,
    gate_weight,
    up_weight,
    down_weight,
):
    n_ep, n_tp = lax.axis_size("ep"), lax.axis_size("tp")
    seqs, width = tokens.shape
    slots = seqs // 2
    rows = n_ep * slots
    columns = gate_weight.shape[1]
    cw = min(512, columns)
    chunks = columns // cw
    quarter = down_weight.shape[1]
    operands = [
        tokens,
        norm_gain.reshape(-1, 128),
        in_weight,
        decay_rate,
        frequency,
        log_step.reshape(1, -1),
        jnp.swapaxes(input_real, 1, 2),
        jnp.swapaxes(input_imag, 1, 2),
        output_real,
        output_imag,
        skip_gain.reshape(1, -1),
        state_real,
        state_imag,
        out_weight,
        ffn_gain.reshape(-1, 128),
        expert_ids.T,
        route_weights.T,
        gate_weight,
        up_weight,
        down_weight,
    ]
    any_spec = pl.BlockSpec(memory_space=pl.ANY)
    smem = pl.BlockSpec(memory_space=pltpu.SMEM)
    vmem = pl.BlockSpec(memory_space=pltpu.VMEM)
    dma = pltpu.SemaphoreType.DMA
    copies = [pltpu.VMEM(value.shape, value.dtype) for value in operands[:15]]
    results = pl.pallas_call(
        functools.partial(kernel, n_ep, n_tp),
        out_shape=(
            jax.ShapeDtypeStruct((seqs, quarter), BF16),
            jax.ShapeDtypeStruct(state_real.shape, F32),
            jax.ShapeDtypeStruct(state_imag.shape, F32),
        ),
        in_specs=[any_spec] * 15 + [smem] * 2 + [any_spec] * 3,
        out_specs=(vmem, vmem, vmem),
        scratch_shapes=copies
        + [
            pltpu.VMEM((chunks, width, cw), BF16),
            pltpu.VMEM((chunks, width, cw), BF16),
            pltpu.VMEM(down_weight.shape, BF16),
            pltpu.VMEM((n_tp, seqs, width), BF16),
            pltpu.VMEM((seqs, width), F32),
            pltpu.VMEM((rows, width), F32),
            pltpu.VMEM((rows, width), BF16),
            pltpu.VMEM((n_ep, slots, width), BF16),
            pltpu.VMEM((n_ep, slots, width), BF16),
            pltpu.VMEM((n_tp, chunks, rows, cw), BF16),
            pltpu.VMEM((rows, quarter), F32),
            pltpu.VMEM((n_ep, slots, quarter), BF16),
            pltpu.VMEM((n_ep, slots, quarter), BF16),
            dma((15,)),
            dma((chunks,)),
            dma((chunks,)),
            dma((n_tp,)),
            dma((n_tp,)),
            dma((n_tp,)),
            dma((n_ep,)),
            dma((n_ep,)),
            dma((n_tp, chunks)),
            dma((n_tp, chunks)),
            dma((n_ep,)),
            dma((n_ep,)),
        ],
        compiler_params=pltpu.CompilerParams(
            collective_id=0, has_side_effects=True, vmem_limit_bytes=60 * 1024 * 1024
        ),
        name="layer",
    )(*operands)
    return pl.pallas_call(
        hand_over,
        out_shape=tuple(jax.ShapeDtypeStruct(r.shape, r.dtype) for r in results),
        in_specs=[vmem] * 3,
        out_specs=(vmem,) * 3,
        name="hand_over",
    )(*results)


def solution(mesh):
    in_specs = (
        P("ep", None),
        P(),
        P(None, "tp"),
        P("tp", None),
        P("tp", None),
        P("tp"),
        P("tp", None, None),
        P("tp", None, None),
        P("tp", None, None),
        P("tp", None, None),
        P("tp"),
        P("ep", "tp", None),
        P("ep", "tp", None),
        P("tp", None),
        P(),
        P(),
        P("ep", None),
        P(None, ("ep", "tp")),
        P(None, ("ep", "tp")),
        P("ep", "tp"),
    )
    out_specs = (P("ep", "tp"), P("ep", "tp", None), P("ep", "tp", None))
    return jax.shard_map(shards, mesh=mesh, in_specs=in_specs, out_specs=out_specs, check_vma=False)
```
